32 devices in a mesh: sp: 8 (over z, core), tp: 4 (over y, x).
Axes of the slice: x: 2, y: 2, z: 4, core: 2. Of those that a mesh axis runs over, the one named last changes fastest.
Arguments:
- layer_input: bfloat16 [2048, 2048], P('sp', 'tp'), may hold values from -6 to 6
- doc_ids: int32 [2048], P('sp'), may hold values from 0 to 1, never falling along the last dimension, each value on 1 to 1536 neighbouring positions
- routes: int32 [2048, 2], P('sp'), may hold values from 0 to 7, all different within a row; in each aligned block of 256 rows (0 to 255, 256 to 511, ...) at most 88 rows name the same one
- route_weight: float32 [2048, 2], P('sp'), may hold values from 0.2 to 2
- pool_weight: bfloat16 [4, 512, 512], replicated, may hold values from -0.25 to 0.25
- pool_scale: float32 [2048], replicated, may hold values from 0.1 to 1.9
- norm1_gain: float32 [2048], replicated, may hold values from 0.3 to 3
- norm1_bias: float32 [2048], replicated, may hold values from -3 to 3
- expert_gate: bfloat16 [8, 2048, 2048], P('sp', None, 'tp'), may hold values from -0.125 to 0.125
- expert_up: bfloat16 [8, 2048, 2048], P('sp', None, 'tp'), may hold values from -0.125 to 0.125
- expert_down: bfloat16 [8, 2048, 2048], P('sp', 'tp'), may hold values from -0.125 to 0.125
- shared_gate: bfloat16 [2048, 1024], P(None, 'tp'), may hold values from -0.125 to 0.125
- shared_up: bfloat16 [2048, 1024], P(None, 'tp'), may hold values from -0.125 to 0.125
- shared_down: bfloat16 [1024, 2048], P('tp'), may hold values from -0.1875 to 0.1875
- norm2_gain: float32 [2048], P('tp'), may hold values from 0.1 to 1.9
- norm2_bias: float32 [2048], P('tp'), may hold values from -3 to 3
Outputs:
- settled: bfloat16 [2048, 2048], P('sp', 'tp')
The draws below stay inside these ranges and needn't reach their ends.
Inputs may be any that keep to these rules, and one draw needn't show every extreme that they name: `routes`: in each aligned block of 256 rows no expert is named by more than 88 picks, a bound that some block reaches. `doc_ids`: never falling along the positions; each document spans 1 to 1536 positions.
All inputs are finite; a program needn't handle non-finite values.
Results may differ from the reference program's by a relative error of at most 0.013.
Values may be sent and summed in bfloat16 or wider, within the bound.
A program may use at most 64 MiB of HBM per device.

```python
import math
import jax
import jax.numpy as jnp
import numpy as np
from jax import lax

D = 2048
GROUPS = 4
GROUP_WIDTH = 512
EXPERT_WIDTH = 2048
SHARED_WIDTH = 1024
TOP_K = 2
TOK_DEV = 256
TOKENS = 2048
EXPERTS = 8
CAPACITY = 88
N_SP = 8
N_TP = 4


def levels(stream_key, dims, cuts, low, top_value):
    level = 1.0
    for axis_at, shards_of in cuts:
        steps = jax.random.uniform(jax.random.fold_in(jax.random.fold_in(stream_key, 6), axis_at), (shards_of,), jnp.float32, low / len(cuts), top_value / len(cuts))
        level = level * jnp.repeat(jnp.exp(steps), dims[axis_at] // shards_of).reshape((-1,) + (1,) * (len(dims) - 1 - axis_at))
    return level


def profile(amount, total, reach, slope):
    weights = [(1 << 20) // math.isqrt(standing ** slope) + 1 for standing in range(2, amount + 1)]
    rest, holding = total - reach - (amount - 1), [1] * (amount - 1)
    while rest > 0:
        movable = [i for i in range(amount - 1) if holding[i] < reach]
        mass, budget = sum([weights[i] for i in movable]), rest
        for i in movable:
            extra = min(reach - holding[i], max(1, budget * weights[i] // mass), rest)
            holding[i] = holding[i] + extra
            rest = rest - extra
    return np.array([reach] + holding)


def uneven_parts(own_key, number_of, total, most, slope):
    if number_of == 2:
        one = jax.random.randint(own_key, (), max(1, total - most), min(most, total - 1) + 1)
        return jnp.stack([one, total - one])
    sizes = jnp.asarray(profile(number_of, total, most, slope), jnp.int32)
    couples = (number_of - 1) // 2
    donor, sink = sizes[1:1 + 2 * couples:2], sizes[2:2 + 2 * couples:2]
    slack = jnp.minimum(donor - 1, most - sink)
    moved = jax.random.randint(jax.random.fold_in(own_key, 1), (couples,), 0, 1 << 20) % (slack + 1)
    sizes = sizes.at[1:1 + 2 * couples:2].set(donor - moved).at[2:2 + 2 * couples:2].set(sink + moved)
    return sizes[jax.random.permutation(jax.random.fold_in(own_key, 2), number_of)]


def routed_block(stream_key, own, number, rows, amount, top, bound, lean):
    sequence = jax.random.permutation(stream_key, amount)
    packed, common = load_shares(amount, rows * top, bound, lean, True), load_shares(amount, rows * top, bound, lean, False)
    places = jnp.arange(amount)

    def named(sizes, rotation):
        used = int((sizes > 0).sum())
        fixed = max(1, used // 4)
        moved = fixed + (places - fixed + rotation * (used - fixed)) % max(1, amount - fixed)
        return jnp.zeros((amount,), jnp.int32).at[sequence[jnp.where(places < fixed, places, moved)]].set(jnp.asarray(sizes, jnp.int32))

    sizes = jnp.where(number % 4 == 0, named(packed, number // 4), named(common, number - number // 4 - 1))
    mixed = jax.random.permutation(jax.random.fold_in(own, 3), amount)
    donor, taker = mixed[0:amount // 2 * 2:2], mixed[1:amount // 2 * 2:2]
    slack = jnp.minimum(sizes[donor] - 1, bound - sizes[taker]) // 2
    slack = jnp.where((donor == sequence[0]) | (taker == sequence[0]) | (sizes[taker] == 0), 0, jnp.maximum(slack, 0))
    moved = jax.random.randint(jax.random.fold_in(own, 4), (amount // 2,), 0, 1 << 20) % (slack + 1)
    sizes = sizes.at[donor].add(-moved).at[taker].add(moved)
    items = jnp.searchsorted(jnp.cumsum(sizes), jnp.arange(rows * top), side="right").astype(jnp.int32)
    listing = items.reshape(top, rows).T
    listing = listing[jax.random.permutation(jax.random.fold_in(own, 1), rows)]
    rotation = jax.random.randint(jax.random.fold_in(own, 2), (rows, 1), 0, top)
    return jnp.take_along_axis(listing, (jnp.arange(top)[None, :] + rotation) % top, axis=1)


def load_shares(number_of, total, reach, slope, full):
    portions = [(1 << 20) // math.isqrt(grade ** slope) + 1 for grade in range(1, number_of + 1)]
    largest = reach if full else min(reach, max(-(-total // number_of), total * portions[0] // sum(portions)))
    least = 1 if total - largest >= number_of - 1 else 0
    holding, spare = [largest] + [least] * (number_of - 1), total - largest - least * (number_of - 1)
    while spare > 0:
        movable = [i for i in range(1, number_of) if holding[i] < largest] or [i for i in range(1, number_of) if holding[i] < reach]
        pool, budget = sum([portions[i] for i in movable]), spare
        for i in movable:
            addition = min(reach - holding[i], max(1, budget * portions[i] // pool), spare)
            holding[i] = holding[i] + addition
            spare = spare - addition
    return np.array(holding)


def noise(rng, extent, deviation, limit, cuts=(), kind=jnp.bfloat16):
    loudness = levels(rng, extent, cuts, -0.22, 0.18) if cuts else 1.0
    array = jax.random.normal(rng, extent, jnp.float32) * deviation * loudness
    return jnp.minimum(jnp.maximum(array, -limit), limit).astype(kind)


def setup_inputs(seed: int = 0) -> dict:
    key_list = jax.random.split(jax.random.key(seed), 17)
    layer_input = noise(key_list[0], (TOKENS, D), 1.0, 6.0, ((0, 8), (1, 4)))
    doc_ids = jnp.searchsorted(jnp.cumsum(uneven_parts(key_list[1], N_SP // 4, TOKENS, 6 * TOK_DEV, 2)), jnp.arange(TOKENS), side="right").astype(jnp.int32)
    routes_keys = jax.random.split(jax.random.fold_in(key_list[2], 1), TOKENS // TOK_DEV)
    routes_turns = jax.random.permutation(jax.random.fold_in(key_list[2], 3), TOKENS // TOK_DEV)
    routes = jax.vmap(lambda own, number: routed_block(jax.random.fold_in(key_list[2], 2), own, number, TOK_DEV, EXPERTS, TOP_K, CAPACITY, 2))(routes_keys, routes_turns).reshape((TOKENS, TOP_K))
    route_weight = jnp.clip(jnp.exp(math.log(2.0) - 2.3025851 * jax.random.uniform(key_list[3], (TOKENS, TOP_K), jnp.float32) ** levels(key_list[3], (TOKENS, TOP_K), ((0, 8),), -0.2, 0.2)), 0.2, 2.0)
    pool_weight = noise(key_list[4], (GROUPS, GROUP_WIDTH, GROUP_WIDTH), GROUP_WIDTH ** -0.5, 0.25)
    pool_scale = jnp.clip(1.0 + 0.18 * jax.random.normal(key_list[5], (D,), jnp.float32), 0.1, 1.9)
    norm1_gain = jnp.clip(jnp.exp(jax.random.uniform(key_list[6], (D,), jnp.float32, math.log(0.3), math.log(3.0))), 0.3, 3.0)
    norm1_bias = noise(key_list[7], (D,), 0.5, 3.0, (), jnp.float32)
    expert_gate = noise(key_list[8], (EXPERTS, D, EXPERT_WIDTH), D ** -0.5, 0.125, ((0, 8), (2, 4)))
    expert_up = noise(key_list[9], (EXPERTS, D, EXPERT_WIDTH), D ** -0.5, 0.125, ((0, 8), (2, 4)))
    expert_down = noise(key_list[10], (EXPERTS, EXPERT_WIDTH, D), EXPERT_WIDTH ** -0.5, 0.125, ((0, 8), (1, 4)))
    shared_gate = noise(key_list[11], (D, SHARED_WIDTH), D ** -0.5, 0.125, ((1, 4),))
    shared_up = noise(key_list[12], (D, SHARED_WIDTH), D ** -0.5, 0.125, ((1, 4),))
    shared_down = noise(key_list[13], (SHARED_WIDTH, D), SHARED_WIDTH ** -0.5, 0.1875, ((0, 4),))
    norm2_gain = jnp.clip(1.0 + 0.18 * jax.random.normal(key_list[14], (D,), jnp.float32), 0.1, 1.9)
    norm2_bias = noise(key_list[15], (D,), 0.5, 3.0, ((0, 4),), jnp.float32)
    return dict(layer_input=layer_input, doc_ids=doc_ids, routes=routes, route_weight=route_weight, pool_weight=pool_weight, pool_scale=pool_scale, norm1_gain=norm1_gain, norm1_bias=norm1_bias, expert_gate=expert_gate, expert_up=expert_up, expert_down=expert_down, shared_gate=shared_gate, shared_up=shared_up, shared_down=shared_down, norm2_gain=norm2_gain, norm2_bias=norm2_bias)


WINDOWS = (2, 4, 8, 16)
HALO_ROWS = 15
RESIDUAL_SCALE = 2.0 ** 0.5
NORM_EPS = 1e-05

def pooled_groups(extended, marks, halo_rows):
    length = extended.shape[0] - halo_rows
    group_width = extended.shape[1] // len(WINDOWS)
    own_mark = marks[halo_rows:]
    values = extended.astype(jnp.float32)
    outputs = []
    for group_index, window in enumerate(WINDOWS):
        section = values[:, group_index * group_width:(group_index + 1) * group_width]
        running = jnp.zeros((length, group_width), jnp.float32)
        members = jnp.zeros((length, 1), jnp.float32)
        for offset in range(window):
            first_row = halo_rows - offset
            inside = (marks[first_row:first_row + length] == own_mark).astype(jnp.float32)[:, None]
            running = running + inside * section[first_row:first_row + length]
            members = members + inside
        outputs.append(running / members - section[halo_rows:])
    return jnp.concatenate(outputs, axis=1).astype(jnp.bfloat16)

def layer_norm_rows(values, gain, bias):
    row_mean = lax.optimization_barrier(jnp.mean(values, axis=1, keepdims=True))
    row_var = lax.optimization_barrier(jnp.mean(values * values, axis=1, keepdims=True)) - row_mean * row_mean
    return (values - row_mean) * lax.rsqrt(row_var + NORM_EPS) * gain + bias

def blockwise_down(hidden, down_weight, pieces):
    piece_width = hidden.shape[1] // pieces

    def add_piece(piece_index, running):
        begin = piece_index.astype(jnp.int32) * piece_width
        part_hidden = lax.dynamic_slice_in_dim(hidden, begin, piece_width, 1)
        part_down = lax.dynamic_slice_in_dim(down_weight, begin, piece_width, 0)
        product = jnp.dot(part_hidden, part_down, preferred_element_type=jnp.float32)
        return running + lax.optimization_barrier(product.astype(jnp.bfloat16)).astype(jnp.float32)
    start_value = jnp.zeros((hidden.shape[0], down_weight.shape[1]), jnp.float32)
    return lax.fori_loop(0, pieces, add_piece, start_value)

def reference(layer_input, doc_ids, routes, route_weight, pool_weight, pool_scale, norm1_gain, norm1_bias, expert_gate, expert_up, expert_down, shared_gate, shared_up, shared_down, norm2_gain, norm2_bias):
    extended = jnp.concatenate([jnp.zeros((HALO_ROWS, D), jnp.bfloat16), layer_input], axis=0)
    marks = jnp.concatenate([jnp.zeros((HALO_ROWS,), jnp.float32), (doc_ids + 1).astype(jnp.float32)])
    mixed = pooled_groups(extended, marks, HALO_ROWS)
    projected = jnp.einsum('tgc,gcd->tgd', mixed.reshape(TOKENS, GROUPS, GROUP_WIDTH).astype(jnp.float32), pool_weight.astype(jnp.float32)).reshape(TOKENS, D)
    first = RESIDUAL_SCALE * layer_input.astype(jnp.float32) + projected * pool_scale
    normed = layer_norm_rows(first, norm1_gain, norm1_bias).astype(jnp.bfloat16)
    picks = routes.reshape(N_SP, TOK_DEV * TOP_K).astype(jnp.int32)
    one_hot = (picks[:, :, None] == jnp.arange(EXPERTS, dtype=jnp.int32)[None, None, :]).astype(jnp.int32)
    ranks = lax.optimization_barrier(jnp.sum((jnp.cumsum(one_hot, axis=1) - one_hot) * one_hot, axis=2)).astype(jnp.int32)
    block_index = jnp.broadcast_to(jnp.arange(N_SP, dtype=jnp.int32)[:, None], picks.shape)
    source_rows = jnp.repeat(normed.reshape(N_SP, TOK_DEV, D), TOP_K, axis=1)
    slots = jnp.zeros((EXPERTS, N_SP, CAPACITY, D), jnp.bfloat16).at[picks, block_index, ranks].set(source_rows)

    def run_expert(operands):
        rows_in, gate_w, up_w, down_w = operands
        slot_rows = rows_in.reshape(N_SP * CAPACITY, D)
        gate_part = jnp.dot(slot_rows, gate_w, preferred_element_type=jnp.float32)
        up_part = jnp.dot(slot_rows, up_w, preferred_element_type=jnp.float32)
        hidden = (jax.nn.silu(gate_part) * up_part).astype(jnp.bfloat16)
        return blockwise_down(hidden, down_w, N_TP).astype(jnp.bfloat16).reshape(N_SP, CAPACITY, D)
    routed = lax.map(run_expert, (slots, expert_gate, expert_up, expert_down))
    returned = routed[picks, block_index, ranks].astype(jnp.float32).reshape(TOKENS, TOP_K, D)
    routed_mix = lax.optimization_barrier(jnp.sum(returned * route_weight[:, :, None], axis=1))
    shared_hidden = (jax.nn.silu(jnp.dot(normed, shared_gate, preferred_element_type=jnp.float32)) * jnp.dot(normed, shared_up, preferred_element_type=jnp.float32)).astype(jnp.bfloat16)
    shared = blockwise_down(shared_hidden, shared_down, N_TP)
    second = RESIDUAL_SCALE * normed.astype(jnp.float32) + routed_mix + shared
    return layer_norm_rows(second, norm2_gain, norm2_bias).astype(jnp.bfloat16)
```

```python
import functools

import jax
import jax.numpy as jnp
from jax import lax
from jax.experimental import pallas as pl
from jax.experimental.pallas import tpu as pltpu
from jax.sharding import PartitionSpec as P

WINDOWS = (2, 4, 8, 16)
HALO_ROWS = 15
RESIDUAL_SCALE = 2.0**0.5
NORM_EPS = 1e-05


def shifted(shard, axis, by):
    size = lax.axis_size(axis)
    pairs = [(i, i + by) for i in range(size) if 0 <= i + by < size]
    return lax.ppermute(shard, axis, pairs)


def pooled_groups(extended, marks, halo_rows):
    length = extended.shape[0] - halo_rows
    group_width = extended.shape[1] // len(WINDOWS)
    own_mark = marks[halo_rows:]
    values = extended.astype(jnp.float32)
    outputs = []
    for group_index, window in enumerate(WINDOWS):
        section = values[:, group_index * group_width : (group_index + 1) * group_width]
        running = jnp.zeros((length, group_width), jnp.float32)
        members = jnp.zeros((length, 1), jnp.float32)
        for offset in range(window):
            first_row = halo_rows - offset
            inside = (marks[first_row : first_row + length] == own_mark).astype(jnp.float32)[
                :, None
            ]
            running = running + inside * section[first_row : first_row + length]
            members = members + inside
        outputs.append(running / members - section[halo_rows:])
    return jnp.concatenate(outputs, axis=1).astype(jnp.bfloat16)


def layer_norm_rows(values, gain, bias):
    row_mean = jnp.mean(values, axis=1, keepdims=True)
    row_var = jnp.mean(values * values, axis=1, keepdims=True) - row_mean * row_mean
    return (values - row_mean) * lax.rsqrt(row_var + NORM_EPS) * gain + bias


def shards(
    layer_input,
    doc_ids,
    routes,
    route_weight,
    pool_weight,
    pool_scale,
    norm1_gain,
    norm1_bias,
    expert_gate,
    expert_up,
    expert_down,
    shared_gate,
    shared_up,
    shared_down,
    norm2_gain,
    norm2_bias,
):
    tokens_here = layer_input.shape[0]
    width_here = layer_input.shape[1]
    doc_marks = (doc_ids + 1).astype(jnp.bfloat16)
    tail_rows, tail_marks = shifted(
        (layer_input[tokens_here - HALO_ROWS :], doc_marks[tokens_here - HALO_ROWS :]), "sp", 1
    )
    extended = jnp.concatenate([tail_rows, layer_input], axis=0)
    marks = jnp.concatenate([tail_marks, doc_marks]).astype(jnp.float32)
    whole = lax.all_gather(extended, "tp", axis=1, tiled=True)
    model_width = whole.shape[1]
    mixed = pooled_groups(whole, marks, HALO_ROWS)
    groups = pool_weight.shape[0]
    group_width = pool_weight.shape[1]
    projected = jnp.einsum(
        "tgc,gcd->tgd",
        mixed.reshape(tokens_here, groups, group_width),
        pool_weight,
        preferred_element_type=jnp.float32,
    ).reshape(tokens_here, model_width)
    first = RESIDUAL_SCALE * whole[HALO_ROWS:].astype(jnp.float32) + projected * pool_scale
    normed = layer_norm_rows(first, norm1_gain, norm1_bias).astype(jnp.bfloat16)
    top = routes.shape[1]
    experts_all = lax.axis_size("sp")
    capacity = (tokens_here * top * 11 + 8 * experts_all - 1) // (8 * experts_all)
    flat_routes = routes.reshape(-1)
    one_hot = (flat_routes[:, None] == jnp.arange(experts_all, dtype=jnp.int32)[None, :]).astype(
        jnp.int32
    )
    ranks = jnp.sum((jnp.cumsum(one_hot, axis=0) - one_hot) * one_hot, axis=1)
    destination = flat_routes * capacity + ranks
    picked_rows = jnp.repeat(normed, top, axis=0)
    send_buffer = (
        jnp.zeros((experts_all * capacity, model_width), jnp.bfloat16)
        .at[destination]
        .set(picked_rows)
    )
    slot_grid = send_buffer.reshape(experts_all, capacity, model_width)
    own_columns = lax.dynamic_slice_in_dim(
        slot_grid, lax.axis_index("tp") * width_here, width_here, 2
    )
    moved = lax.all_to_all(own_columns, "sp", split_axis=0, concat_axis=0, tiled=True)
    arrived = lax.all_gather(moved, "tp", axis=2, tiled=True)
    arrived_rows = arrived.reshape(-1, model_width)
    gate_part = jnp.dot(arrived_rows, expert_gate[0], preferred_element_type=jnp.float32)
    up_part = jnp.dot(arrived_rows, expert_up[0], preferred_element_type=jnp.float32)
    expert_hidden = (jax.nn.silu(gate_part) * up_part).astype(jnp.bfloat16)
    routed_partial = jnp.dot(expert_hidden, expert_down[0], preferred_element_type=jnp.float32)
    shared_gate_part = jnp.dot(normed, shared_gate, preferred_element_type=jnp.float32)
    shared_up_part = jnp.dot(normed, shared_up, preferred_element_type=jnp.float32)
    shared_hidden = (jax.nn.silu(shared_gate_part) * shared_up_part).astype(jnp.bfloat16)
    shared_partial = jnp.dot(shared_hidden, shared_down, preferred_element_type=jnp.float32)
    routed_sum, shared_sum = (
        lax.psum_scatter(
            routed_partial.astype(jnp.bfloat16), "tp", scatter_dimension=1, tiled=True
        ).astype(jnp.float32),
        lax.psum_scatter(
            shared_partial.astype(jnp.bfloat16), "tp", scatter_dimension=1, tiled=True
        ).astype(jnp.float32),
    )
    routed_here = routed_sum.astype(jnp.bfloat16).reshape(experts_all, capacity, width_here)
    returned = lax.all_to_all(routed_here, "sp", split_axis=0, concat_axis=0, tiled=True)
    returned_rows = returned.reshape(experts_all * capacity, width_here)
    picked_out = (
        returned_rows[destination].astype(jnp.float32).reshape(tokens_here, top, width_here)
    )
    routed_mix = jnp.sum(picked_out * route_weight[:, :, None], axis=1)
    own_normed = lax.dynamic_slice_in_dim(
        normed, lax.axis_index("tp") * width_here, width_here, 1
    ).astype(jnp.float32)
    second = RESIDUAL_SCALE * own_normed + routed_mix + shared_sum
    row_total, row_squares = lax.psum(
        (jnp.sum(second, axis=1), jnp.sum(second * second, axis=1)), "tp"
    )
    row_mean = row_total / model_width
    row_var = row_squares / model_width - row_mean * row_mean
    scaled = (second - row_mean[:, None]) * lax.rsqrt(row_var + NORM_EPS)[:, None]
    return (scaled * norm2_gain + norm2_bias).astype(jnp.bfloat16)


MESH_ID = pl.DeviceIdType.MESH
HALO = 16
LANES = 128
F32 = jnp.float32
BF16 = jnp.bfloat16
ORDER = (
    "G0", "G1", "R0", "G2", "R1", "G3", "R2", "R3", "G4", "G5", "D3", "E0", "S0", "S1",
    "H0", "E1", "H1", "R4", "R5", "G6", "G7", "E2", "S4", "S5", "R6", "H2", "R7", "F4",
    "F5", "E3", "S6", "S7", "S2", "S3", "T4", "T5", "H3", "F6", "F7", "F2", "F3", "F1",
    "F0", "T6", "T7", "T2", "T3", "T1", "M2", "T0", "M1", "M3", "M0",
)


def fused_kernel(
    dims,
    x_hbm,
    doc_hbm,
    route_hbm,
    weight_hbm,
    scale_hbm,
    gain1_hbm,
    bias1_hbm,
    gain2_hbm,
    bias2_hbm,
    pool_hbm,
    gate_hbm,
    up_hbm,
    down_hbm,
    sgate_hbm,
    sup_hbm,
    sdown_hbm,
    out_ref,
    x_ref,
    doc_ref,
    route_ref,
    weight_ref,
    scale_ref,
    gain1_ref,
    bias1_ref,
    gain2_ref,
    bias2_ref,
    pool_w,
    gate_w,
    up_w,
    down_w,
    sgate_w,
    sup_w,
    sdown_w,
    halo_x,
    halo_s,
    halo_c,
    disp,
    disp_t,
    picks,
    wsend,
    wrecv,
    stat_send,
    stat_recv,
    acc,
    sbuf,
    xs,
    pbuf,
    pown,
    rdx,
    rdy,
    fx,
    fy,
    rsend,
    rback,
    send_sems,
    recv_sems,
    load_sems,
):
    experts, tps, cap, pad, windows = dims
    rows, width = x_ref.shape
    half = width // 2
    chips = experts // 2
    model_width = width * tps
    sp = lax.axis_index("sp")
    tp = lax.axis_index("tp")
    chip = sp // 2
    core = sp % 2
    xn = tp + 1 - 2 * (tp % 2)
    yn = lax.rem(tp + 2, tps)
    diag = xn + 2 - 4 * (xn // 2)
    at_q = (tp, xn, yn, diag)
    bits = [1 << i for i in range(chips.bit_length() - 1)]

    def peer(j):
        across = 0
        for bit in bits:
            own = (chip // bit) % 2
            across = across + bit * (1 - own if (j // 2) & bit else own)
        return across * 2 + (1 - core if j % 2 else core)

    counter = [0]

    def remote(src, dst, device):
        k = counter[0]
        counter[0] += 1
        return pltpu.make_async_remote_copy(
            src_ref=src,
            dst_ref=dst,
            send_sem=send_sems.at[k],
            recv_sem=recv_sems.at[k],
            device_id=device,
            device_id_type=MESH_ID,
        )

    barrier = pltpu.get_barrier_semaphore()
    for q in range(1, tps):
        pl.semaphore_signal(barrier, inc=1, device_id=(sp, at_q[q]), device_id_type=MESH_ID)
    for j in range(1, experts):
        pl.semaphore_signal(barrier, inc=1, device_id=(peer(j), tp), device_id_type=MESH_ID)

    loads = {}
    load_count = [0]

    def load(name, src, dst):
        k = load_count[0]
        load_count[0] += 1
        copy = pltpu.make_async_copy(src, dst, load_sems.at[k])
        copy.start()
        loads.setdefault(name, []).append(copy)

    def loaded(name):
        for copy in loads[name]:
            copy.wait()

    def of_q(ref, q):
        return ref[:, pl.ds(pl.multiple_of(at_q[q] * width, width), width)]

    own_block = pl.ds(pl.multiple_of(tp * width, width), width)
    load("x", x_hbm, x_ref)
    load("doc", doc_hbm, doc_ref)
    load("route", route_hbm, route_ref)
    load("route", weight_hbm, weight_ref)
    load("pool", pool_hbm.at[tp], pool_w)
    load("pool", scale_hbm.at[:, own_block], scale_ref)
    load("norm", gain1_hbm, gain1_ref)
    load("norm", bias1_hbm, bias1_ref)
    load("norm", gain2_hbm, gain2_ref)
    load("norm", bias2_hbm, bias2_ref)
    for q in range(tps):
        block = pl.ds(pl.multiple_of(at_q[q] * width, width), width)
        load("in", gate_hbm.at[0, block, :], gate_w.at[q])
        load("in", up_hbm.at[0, block, :], up_w.at[q])
        load("in", sgate_hbm.at[block, :], sgate_w.at[q])
        load("in", sup_hbm.at[block, :], sup_w.at[q])
        load("down", down_hbm.at[0, :, block], down_w.at[q])
        load("down", sdown_hbm.at[:, block], sdown_w.at[q])

    loaded("doc")
    sub8 = lax.broadcasted_iota(jnp.int32, (8, rows), 0)
    doc_row = jnp.where(sub8 == 0, doc_ref[...].astype(F32), 0.0)
    docs = jnp.broadcast_to(doc_row.T[:, 0:1], (rows, LANES))
    halo_s[...] = docs[rows - HALO :]
    loaded("x")

    following = lax.rem(sp + 1, experts)
    halo_copies = [
        remote(x_ref.at[pl.ds(rows - HALO, HALO)], halo_x, (following, tp)),
        remote(halo_s, halo_c, (following, tp)),
    ]
    with jax.named_scope("barrier"):
        pl.semaphore_wait(barrier, tps - 1 + experts - 1)

    @pl.when(sp < experts - 1)
    def _():
        for copy in halo_copies:
            copy.start()

    window = jnp.int32(windows[0])
    for index in range(1, len(windows)):
        window = jnp.where(tp == index, windows[index], window)

    def pooled(values, marks):
        running = values
        members = jnp.ones(marks.shape, F32)
        step = 1
        while step < max(windows):
            same = (marks == pltpu.roll(marks, step, 0)) & (step < window)
            running = running + jnp.where(same[:, 0:1], pltpu.roll(running, step, 0), 0.0)
            members = members + jnp.where(same, pltpu.roll(members, step, 0), 0.0)
            step *= 2
        return (running / members[:, 0:1] - values).astype(BF16)

    def projected(values, mixed):
        product = jnp.dot(mixed, pool_w[...], preferred_element_type=F32)
        return (2.0**0.5) * values + product * scale_ref[...]

    value = x_ref[...].astype(F32)
    mixed = pooled(value, docs)
    loaded("pool")
    first = projected(value, mixed)
    sums = [
        jnp.sum(first, axis=1, keepdims=True),
        jnp.sum(first * first, axis=1, keepdims=True),
    ]

    lane = lax.broadcasted_iota(jnp.int32, (rows, LANES), 1)
    loaded("route")
    routes = route_ref[...].astype(F32)
    weights = weight_ref[...]
    table = jnp.where(
        sub8 == 0,
        routes[0:1],
        jnp.where(
            sub8 == 1,
            routes[1:2],
            jnp.where(sub8 == 2, weights[0:1], jnp.where(sub8 == 3, weights[1:2], 0.0)),
        ),
    )
    cols = table.T
    route = [(cols[:, k : 1 + k] + 0.5).astype(jnp.int32) for k in range(2)]
    named = [lane == route[k] for k in range(2)]
    count = named[0].astype(F32) + named[1].astype(F32)
    earlier = (
        lax.broadcasted_iota(jnp.int32, (rows, rows), 0)
        > lax.broadcasted_iota(jnp.int32, (rows, rows), 1)
    ).astype(F32)
    rank = jnp.dot(earlier.astype(BF16), count.astype(BF16), preferred_element_type=F32)
    differs = jnp.where(lane % 2 == core, 0, 1)
    for bit in bits:
        differs = differs + jnp.where((lane // (2 * bit)) % 2 == (chip // bit) % 2, 0, 2 * bit)
    place = (rank + 0.5).astype(jnp.int32) + differs * pad
    dest = [
        jnp.sum(jnp.where(named[k], place, 0).astype(F32), axis=1, keepdims=True) for k in range(2)
    ]
    wide = (place + differs * (LANES - pad)).astype(F32)
    dest_wide = [
        jnp.sum(jnp.where(named[k], wide, 0.0), axis=1, keepdims=True) for k in range(2)
    ]
    both = jnp.where(lane == 0, dest[0], jnp.where(lane == 1, dest[1], 0.0))
    both_rows = both.T
    slot_row = lax.broadcasted_iota(jnp.int32, (experts * pad, rows), 0)
    dest_row = [(both_rows[k : k + 1, :] + 0.5).astype(jnp.int32) for k in range(2)]
    disp[...] = jnp.where(
        (slot_row == dest_row[0]) | (slot_row == dest_row[1]), 1.0, 0.0
    ).astype(BF16)
    dest_col = [(dest[k] + 0.5).astype(jnp.int32) for k in range(2)]

    @pl.when(sp > 0)
    def _():
        with jax.named_scope("halo_wait"):
            for copy in halo_copies:
                copy.wait_recv()

    halo_docs = jnp.where(sp == 0, -1.0, halo_c[...])
    early = jnp.concatenate([halo_x[...].astype(F32), value[:HALO]], axis=0)
    early_docs = jnp.concatenate([halo_docs, docs[:HALO]], axis=0)
    early_mixed = pooled(early, early_docs)[HALO:]
    early_first = projected(value[:HALO], early_mixed)
    first = jnp.concatenate([early_first, first[HALO:]], axis=0)
    sums = [
        jnp.concatenate([jnp.sum(early_first, axis=1, keepdims=True), sums[0][HALO:]], axis=0),
        jnp.concatenate(
            [jnp.sum(early_first * early_first, axis=1, keepdims=True), sums[1][HALO:]], axis=0
        ),
    ]
    centred = (first - sums[0] / width).astype(BF16)
    acc[...] = first

    def exchange_start(total, squares, slot):
        tile = jnp.where(lane == 0, total, jnp.where(lane == 1, squares, 0.0))
        own = tile.T[0:8]
        stat_send[slot] = own
        copies = []
        for q in range(1, tps):
            copies.append(remote(stat_send.at[slot], stat_recv.at[slot, q], (sp, at_q[q])))
            copies[-1].start()
        return own, copies

    def exchange_end(own, copies, slot):
        with jax.named_scope("stat_wait%d" % slot):
            for copy in copies:
                copy.wait_recv()
        shares = [own] + [stat_recv[slot, q] for q in range(1, tps)]
        whole = shares[0]
        for q in range(1, tps):
            whole = whole + shares[q]
        mean = whole[0:1] / model_width
        var = whole[1:2] / model_width - mean * mean
        inverse = lax.rsqrt(var + 1e-5)
        back = jnp.where(sub8 == 0, mean, jnp.where(sub8 == 1, inverse, 0.0)).T
        shifts = [share[0:1] / width - mean for share in shares]
        return back[:, 0:1], back[:, 1:2], inverse, shifts

    moves, to_x, to_y, via_x, via_y = {}, {}, {}, {}, {}
    half_x, half_y, full_x, full_y, back = {}, {}, {}, {}, {}
    weight_copies = {}
    low, high = pl.ds(0, half), pl.ds(half, half)

    def unit(ref, q, j, columns=None):
        if columns is None:
            return ref.at[q, j, pl.ds(0, cap)]
        return ref.at[q, j, pl.ds(0, cap), columns]

    def plain(ref, j):
        return ref.at[j, pl.ds(0, cap)]

    def gather(j):
        if j:
            with jax.named_scope("w_moves#%d" % j):
                moves[j].wait_recv()
        to_x[j] = remote(unit(xs, 0, j), unit(xs, 1, j), (sp, xn))
        to_x[j].start()
        to_y[j] = remote(unit(xs, 0, j), unit(xs, 2, j), (sp, yn))
        to_y[j].start()

    def relay(j):
        with jax.named_scope("w_to#%d" % j):
            to_x[j].wait_recv()
        via_y[j] = remote(unit(xs, 1, j, low), unit(xs, 3, j, low), (sp, yn))
        via_y[j].start()
        with jax.named_scope("w_to#%d" % j):
            to_y[j].wait_recv()
        via_x[j] = remote(unit(xs, 2, j, high), unit(xs, 3, j, high), (sp, xn))
        via_x[j].start()

    expert_started = []
    partials = {}

    def expert(c):
        for j in (2 * c, 2 * c + 1):
            with jax.named_scope("w_via#%d" % j):
                via_x[j].wait_recv()
                via_y[j].wait_recv()
                if j:
                    weight_copies[j].wait_recv()
        if not expert_started:
            loaded("in")
        size = 2 * pad
        tiles = [wrecv[2 * c + b].T[0:pad] for b in range(2)]
        slot = jnp.concatenate(tiles, axis=0)
        acts = []
        for q in range(tps):
            raw = xs[q, 2 * c : 2 * c + 2].reshape(size, width).astype(F32)
            raw = (raw + slot[:, 3 + q : 4 + q]) * slot[:, 2:3]
            acts.append((raw * of_q(gain1_ref, q) + of_q(bias1_ref, q)).astype(BF16))

        def project(w):
            total = jnp.dot(acts[0], w[0], preferred_element_type=F32)
            for q in range(1, tps):
                total = total + jnp.dot(acts[q], w[q], preferred_element_type=F32)
            return total

        hidden = (jax.nn.silu(project(gate_w)) * project(up_w) * slot[:, 0:1]).astype(BF16)
        shared = (jax.nn.silu(project(sgate_w)) * project(sup_w) * slot[:, 1:2]).astype(BF16)
        if not expert_started:
            loaded("down")
            expert_started.append(True)

        def partial(q):
            return jnp.dot(hidden, down_w[q], preferred_element_type=F32) + jnp.dot(
                shared, sdown_w[q], preferred_element_type=F32
            )

        two = slice(2 * c, 2 * c + 2)
        pbuf[3, two] = partial(3).astype(BF16).reshape(2, pad, width)
        partials[c] = partial

    def hand_over(c):
        two = slice(2 * c, 2 * c + 2)
        pbuf[1, two] = partials[c](1).astype(BF16).reshape(2, pad, width)
        pbuf[2, two] = partials[c](2).astype(BF16).reshape(2, pad, width)
        pown[two] = partials[c](0).reshape(2, pad, width)

    def spread(j):
        half_x[j] = remote(unit(pbuf, 3, j, low), plain(rdx, j), (sp, xn))
        half_x[j].start()
        half_y[j] = remote(unit(pbuf, 3, j, high), plain(rdy, j), (sp, yn))
        half_y[j].start()

    def fold(j):
        with jax.named_scope("w_half#%d" % j):
            half_x[j].wait_recv()
        pbuf[2, j, :, :half] = (pbuf[2, j, :, :half].astype(F32) + rdx[j].astype(F32)).astype(BF16)
        full_y[j] = remote(unit(pbuf, 2, j), plain(fy, j), (sp, yn))
        full_y[j].start()
        with jax.named_scope("w_half#%d" % j):
            half_y[j].wait_recv()
        pbuf[1, j, :, half:] = (pbuf[1, j, :, half:].astype(F32) + rdy[j].astype(F32)).astype(BF16)
        full_x[j] = remote(unit(pbuf, 1, j), plain(fx, j), (sp, xn))
        full_x[j].start()

    def turn(j):
        with jax.named_scope("w_full#%d" % j):
            full_x[j].wait_recv()
            full_y[j].wait_recv()
        total = (pown[j] + fx[j].astype(F32) + fy[j].astype(F32)).astype(BF16)
        if j == 0:
            rback[0] = total
        else:
            rsend[j] = total
            back[j] = remote(plain(rsend, j), plain(rback, j), (peer(j), tp))
            back[j].start()

    def merge(c):
        for j in (2 * c, 2 * c + 1):
            if j:
                with jax.named_scope("w_back#%d" % j):
                    back[j].wait_recv()
        slots = rback[2 * c : 2 * c + 2].reshape(2 * pad, width)
        inner = lax.broadcasted_iota(jnp.int32, (2, pad, width), 1).reshape(2 * pad, width)
        slots = jnp.where(inner < cap, slots.astype(F32), 0.0).astype(BF16)
        acc[...] += jnp.dot(disp_t[c], slots, preferred_element_type=F32)

    own1, stat_copies = exchange_start(sums[0], sums[1], 0)
    inner_chip = ((chip + 1) // 2) % 2 == 1
    for c in range(chips):
        part = jnp.dot(
            disp[c * 2 * pad : (c + 1) * 2 * pad, :], centred, preferred_element_type=F32
        ).astype(BF16)
        for b in range(2):
            j = 2 * c + b
            piece = part[b * pad : (b + 1) * pad]
            if j == 0:
                xs[0, 0] = piece
                gather(0)
            else:
                sbuf[j] = piece
                moves[j] = remote(plain(sbuf, j), xs.at[0, j, pl.ds(0, cap)], (peer(j), tp))
                if c < 2:
                    moves[j].start()

    @pl.when(inner_chip)
    def _():
        for j in (6, 7):
            moves[j].start()

    pick_lane = lax.broadcasted_iota(jnp.int32, (rows, experts * LANES), 1)
    for k in range(2):
        spot = (dest_wide[k] + 0.5).astype(jnp.int32)
        picks[k * rows : (k + 1) * rows] = jnp.where(pick_lane == spot, 1.0, 0.0).astype(BF16)
    with jax.named_scope("G1"):
        gather(1)
    mean, inverse, inverse_row, shifts = exchange_end(own1, stat_copies, 0)

    def slot_rows(weight_row, flag):
        out = jnp.where(sub8 == 0, weight_row, jnp.where(sub8 == 1, flag, 0.0))
        out = jnp.where(sub8 == 2, inverse_row, out)
        for q in range(tps):
            out = jnp.where(sub8 == 3 + q, shifts[q], out)
        return out

    left = jnp.concatenate([slot_rows(weights[0:1], 1.0), slot_rows(weights[1:2], 0.0)], axis=1)
    slot_values = jnp.zeros((8, experts * LANES), F32)
    for _ in range(3):
        piece = left.astype(BF16)
        slot_values = slot_values + jnp.dot(piece, picks[...], preferred_element_type=F32)
        left = left - piece.astype(F32)
    for j in range(experts):
        tile = slot_values[:, j * LANES : (j + 1) * LANES]
        if j == 0:
            wrecv[0] = tile
        else:
            wsend[j] = tile
            weight_copies[j] = remote(wsend.at[j], wrecv.at[j], (peer(j), tp))
            weight_copies[j].start()

    @pl.when(inner_chip)
    def _():
        for j in (4, 5):
            moves[j].start()

    @pl.when(jnp.logical_not(inner_chip))
    def _():
        for j in (4, 5):
            moves[j].start()

    loaded("norm")
    normed = ((acc[...] - mean) * inverse * of_q(gain1_ref, 0) + of_q(bias1_ref, 0)).astype(BF16)
    acc[...] = (2.0**0.5) * normed.astype(F32)
    slot_lane = lax.broadcasted_iota(jnp.int32, (rows, 2 * pad), 1)
    for c in range(chips):
        here = slot_lane + c * 2 * pad
        disp_t[c] = jnp.where((here == dest_col[0]) | (here == dest_col[1]), 1.0, 0.0).astype(BF16)

    def depart(pair):
        @pl.when(jnp.logical_not(inner_chip))
        def _():
            for j in (2 * pair, 2 * pair + 1):
                moves[j].start()

    stages = {
        "D": depart, "G": gather, "R": relay, "E": expert, "H": hand_over, "S": spread, "F": fold, "T": turn, "M": merge
    }
    for step in ORDER:
        if step in ("G0", "G1"):
            continue
        with jax.named_scope(step):
            stages[step[0]](int(step[1:]))

    second = acc[...]
    own2, stat_copies2 = exchange_start(
        jnp.sum(second, axis=1, keepdims=True), jnp.sum(second * second, axis=1, keepdims=True), 1
    )
    mean2, inverse2, _, _ = exchange_end(own2, stat_copies2, 1)
    with jax.named_scope("final"):
        out_ref[...] = ((second - mean2) * inverse2 * gain2_ref[...] + bias2_ref[...]).astype(BF16)

    @pl.when(sp < experts - 1)
    def _():
        for copy in halo_copies:
            copy.wait_send()

    for copy in stat_copies + stat_copies2:
        copy.wait_send()
    for group in (weight_copies, moves, to_x, to_y, via_x, via_y):
        for copy in group.values():
            copy.wait_send()
    for group in (half_x, half_y, full_x, full_y, back):
        for copy in group.values():
            copy.wait_send()


def fused_shards(
    layer_input,
    doc_ids,
    routes,
    route_weight,
    pool_weight,
    pool_scale,
    norm1_gain,
    norm1_bias,
    expert_gate,
    expert_up,
    expert_down,
    shared_gate,
    shared_up,
    shared_down,
    norm2_gain,
    norm2_bias,
):
    rows, width = layer_input.shape
    experts = lax.axis_size("sp")
    tps = lax.axis_size("tp")
    top = routes.shape[1]
    cap = (rows * top * 11 + 8 * experts - 1) // (8 * experts)
    pad = -(-cap // 16) * 16
    hidden = expert_gate.shape[2]
    shared = shared_gate.shape[1]
    slots = (experts, pad, width)
    half = (experts, pad, width // 2)
    copies = 2 + 3 * (experts - 1) + 2 * (tps - 1) + 8 * experts
    vmem = pl.BlockSpec(memory_space=pltpu.VMEM)
    hbm = pl.BlockSpec(memory_space=pl.ANY)
    return pl.pallas_call(
        functools.partial(fused_kernel, (experts, tps, cap, pad, WINDOWS)),
        out_shape=jax.ShapeDtypeStruct((rows, width), BF16),
        in_specs=[hbm] * 16,
        out_specs=vmem,
        scratch_shapes=[
            pltpu.VMEM((rows, width), BF16),
            pltpu.VMEM((1, rows), jnp.int32),
            pltpu.VMEM((top, rows), jnp.int32),
            pltpu.VMEM((top, rows), F32),
            pltpu.VMEM((1, width), F32),
            pltpu.VMEM((1, tps * width), F32),
            pltpu.VMEM((1, tps * width), F32),
            pltpu.VMEM((1, width), F32),
            pltpu.VMEM((1, width), F32),
            pltpu.VMEM((width, width), BF16),
            pltpu.VMEM((tps, width, hidden), BF16),
            pltpu.VMEM((tps, width, hidden), BF16),
            pltpu.VMEM((tps, hidden, width), BF16),
            pltpu.VMEM((tps, width, shared), BF16),
            pltpu.VMEM((tps, width, shared), BF16),
            pltpu.VMEM((tps, shared, width), BF16),
            pltpu.VMEM((HALO, width), BF16),
            pltpu.VMEM((HALO, LANES), F32),
            pltpu.VMEM((HALO, LANES), F32),
            pltpu.VMEM((experts * pad, rows), BF16),
            pltpu.VMEM((experts // 2, rows, 2 * pad), BF16),
            pltpu.VMEM((top * rows, experts * LANES), BF16),
            pltpu.VMEM((experts, 8, LANES), F32),
            pltpu.VMEM((experts, 8, LANES), F32),
            pltpu.VMEM((2, 8, rows), F32),
            pltpu.VMEM((2, tps, 8, rows), F32),
            pltpu.VMEM((rows, width), F32),
            pltpu.VMEM(slots, BF16),
            pltpu.VMEM((tps,) + slots, BF16),
            pltpu.VMEM((tps,) + slots, BF16),
            pltpu.VMEM(slots, F32),
            pltpu.VMEM(half, BF16),
            pltpu.VMEM(half, BF16),
            pltpu.VMEM(slots, BF16),
            pltpu.VMEM(slots, BF16),
            pltpu.VMEM(slots, BF16),
            pltpu.VMEM(slots, BF16),
            pltpu.SemaphoreType.DMA((copies,)),
            pltpu.SemaphoreType.DMA((copies,)),
            pltpu.SemaphoreType.DMA((10 + 6 * tps,)),
        ],
        compiler_params=pltpu.CompilerParams(
            collective_id=0, has_side_effects=True, vmem_limit_bytes=60 * 1024 * 1024
        ),
    )(
        layer_input,
        doc_ids.reshape(1, rows),
        routes.T,
        route_weight.T,
        pool_scale.reshape(1, -1),
        norm1_gain.reshape(1, -1),
        norm1_bias.reshape(1, -1),
        norm2_gain.reshape(1, -1),
        norm2_bias.reshape(1, -1),
        pool_weight,
        expert_gate,
        expert_up,
        expert_down,
        shared_gate,
        shared_up,
        shared_down,
    )


def layer(*arrays):
    layer_input, pool_weight = arrays[0], arrays[4]
    one_group_each = layer_input.shape[1] == pool_weight.shape[1]
    if one_group_each and lax.axis_size("tp") == 4 and lax.axis_size("sp") == 8:
        return fused_shards(*arrays)
    return shards(*arrays)


def solution(mesh):
    in_specs = (
        P("sp", "tp"),
        P("sp"),
        P("sp", None),
        P("sp", None),
        P(),
        P(),
        P(),
        P(),
        P("sp", None, "tp"),
        P("sp", None, "tp"),
        P("sp", "tp", None),
        P(None, "tp"),
        P(None, "tp"),
        P("tp", None),
        P("tp"),
        P("tp"),
    )
    out_specs = P("sp", "tp")
    return jax.shard_map(layer, mesh=mesh, in_specs=in_specs, out_specs=out_specs, check_vma=False)
```
